32 devices in a mesh: grp: 2 (over y), kv: 4 (over z), tp: 4 (over x, core).
Axes of the slice: x: 2, y: 2, z: 4, core: 2. Of those that a mesh axis runs over, the one named last changes fastest.
Arguments:
- hidden: bfloat16 [256, 4096], P('grp', 'kv'), parts along dimension 0, may hold values from -64 to 64
- norm_gain: bfloat16 [4096], replicated, may hold values from 0.099609375 to 1.8984375
- w_query: bfloat16 [4096, 2048], P('kv', 'tp'), may hold values from -0.09375 to 0.09375
- w_key: bfloat16 [4096, 2048], P('kv', 'tp'), may hold values from -0.09375 to 0.09375
- w_value: bfloat16 [4096, 2048], P('kv', 'tp'), may hold values from -0.09375 to 0.09375
- w_gate: bfloat16 [4096, 2048], P('kv', 'tp'), may hold values from -0.09375 to 0.09375
- w_decay: bfloat16 [4096, 16], P(None, 'tp'), may hold values from -0.09375 to 0.09375
- w_write: bfloat16 [4096, 16], P(None, 'tp'), may hold values from -0.09375 to 0.09375
- decay_rate: float32 [16], P('tp'), may hold values from 0.02 to 1
- head_gain: bfloat16 [128], replicated, may hold values from 0.099609375 to 1.8984375
- w_output: bfloat16 [2048, 4096], P('tp', 'kv'), may hold values from -0.125 to 0.125
- state: float32 [64, 16, 16384], P(('grp', 'kv'), 'tp'), parts along dimension 0, may hold values from -6 to 6
- prev_keys: bfloat16 [64, 4, 2048], P(('grp', 'kv'), None, 'tp'), parts along dimension 0, may hold values from -6 to 6
- prev_values: bfloat16 [64, 4, 2048], P(('grp', 'kv'), None, 'tp'), parts along dimension 0, may hold values from -6 to 6
- prev_decay: float32 [64, 4, 16], P(('grp', 'kv'), None, 'tp'), parts along dimension 0, may hold values from -1 to -0.02
- prev_write: float32 [64, 4, 16], P(('grp', 'kv'), None, 'tp'), parts along dimension 0, may hold values from 0.05 to 0.95
- accepted: int32 [64], P(('grp', 'kv')), parts along dimension 0, may hold values from 0 to 4
Outputs:
- mixed: bfloat16 [256, 4096], P('grp', 'kv'), parts along dimension 0
- state_out: float32 [64, 16, 16384], P(('grp', 'kv'), 'tp'), parts along dimension 0
The draws below stay inside these ranges and needn't reach their ends.
There are 2 independent parts, one for each index of `grp`. The reference program is written for one: setup_inputs(seed, part) draws one part's arguments, and reference() takes and returns one part's arrays. A program takes and returns all parts, laid end to end along the dimension named above; an argument that names none is the same for every part. Nothing has to cross between parts.
All inputs are finite; a program needn't handle non-finite values.
Results may differ from the reference program's by a relative error of at most 0.0069.
Values may be sent and summed in bfloat16 or wider, within the bound.
No kernel may reach another device: no remote copies, remote signals or barrier semaphores. Data moves between devices by JAX's collectives and lax.ppermute only.
A program may use at most 64 MiB of HBM per device.

```python
import math
import jax
import jax.numpy as jnp
from jax import lax

D = 4096
H = 16
DK = 128
PROP = 4
SEQS = 32
TOKENS = 128
HID = 2048


def draw_hidden(key, part):
    key_rows, key_cols, key_base = jax.random.split(jax.random.fold_in(key, 11), 3)
    columns = jnp.arange(D, dtype=jnp.float32)
    column_scale = jnp.exp(math.log(3.0) * columns / D + jax.random.uniform(key_cols, (D,), jnp.float32, -0.35, 0.35))
    row_scale = jnp.exp(jax.random.uniform(key_rows, (TOKENS, 1), jnp.float32, 0.0, math.log(10.0)))
    base = jax.random.normal(key_base, (TOKENS, D), jnp.float32)
    base = jnp.clip(base, -5.0, 5.0)
    return jnp.clip(0.3 * base * row_scale * column_scale, -64.0, 64.0).astype(jnp.bfloat16)


def plant(drawn, own_key, low, high):
    spot = [jax.random.randint(jax.random.fold_in(own_key, axis), (), 0, length) for axis, length in enumerate(drawn.shape)]
    widest = drawn.shape.index(max(drawn.shape))
    beside = spot[:widest] + [(spot[widest] + 1) % drawn.shape[widest]] + spot[widest + 1:]
    return drawn.at[tuple(spot)].set(low).at[tuple(beside)].set(high)


def block_levels(own_key, extent, pieces, least, top_value):
    loudness = 1.0
    for axis_at, parts in pieces:
        steps = jax.random.uniform(jax.random.fold_in(jax.random.fold_in(own_key, 6), axis_at), (parts,), jnp.float32, least / len(pieces), top_value / len(pieces))
        loudness = loudness * jnp.repeat(jnp.exp(steps), extent[axis_at] // parts).reshape((-1,) + (1,) * (len(extent) - 1 - axis_at))
    return loudness


def normal_values(key, shape, spread, most, cuts=(), kind=jnp.bfloat16):
    values = spread * jax.random.normal(key, shape, jnp.float32)
    if cuts:
        values = values * block_levels(key, shape, cuts, -0.22, 0.18)
    return jnp.clip(values, -most, most).astype(kind)


def setup_inputs(seed: int = 0, part: int = 0) -> dict:
    arg_keys = jax.random.split(jax.random.key(seed), 18)
    part_splits = jax.random.split(jax.random.fold_in(arg_keys[17], part), 18)
    return {
        "hidden": draw_hidden(jax.random.fold_in(jax.random.fold_in(arg_keys[17], part), 71), part),
        "norm_gain": jnp.clip(1.0 + 0.18 * jax.random.normal(arg_keys[1], (D,), jnp.float32), 0.099609375, 1.8984375).astype(jnp.bfloat16),
        "w_query": normal_values(arg_keys[2], (D, HID), D ** -0.5, 0.09375, ((0, 4), (1, 4))),
        "w_key": normal_values(arg_keys[3], (D, HID), D ** -0.5, 0.09375, ((0, 4), (1, 4))),
        "w_value": normal_values(arg_keys[4], (D, HID), D ** -0.5, 0.09375, ((0, 4), (1, 4))),
        "w_gate": normal_values(arg_keys[5], (D, HID), D ** -0.5, 0.09375, ((0, 4), (1, 4))),
        "w_decay": normal_values(arg_keys[6], (D, H), D ** -0.5, 0.09375, ((1, 4),)),
        "w_write": normal_values(arg_keys[7], (D, H), D ** -0.5, 0.09375, ((1, 4),)),
        "decay_rate": jnp.clip(jnp.exp(math.log(1.0) - 3.912023 * jax.random.uniform(arg_keys[8], (H,), jnp.float32) ** block_levels(arg_keys[8], (H,), ((0, 4),), -0.2, 0.2)), 0.02, 1.0),
        "head_gain": jnp.clip(1.0 + 0.18 * jax.random.normal(arg_keys[9], (DK,), jnp.float32), 0.099609375, 1.8984375).astype(jnp.bfloat16),
        "w_output": normal_values(arg_keys[10], (HID, D), HID ** -0.5, 0.125, ((0, 4), (1, 4))),
        "state": normal_values(part_splits[11], (SEQS, H, DK * DK), 1.0, 6.0, ((0, 4), (1, 4)), jnp.float32),
        "prev_keys": normal_values(part_splits[12], (SEQS, PROP, HID), 1.0, 6.0, ((0, 4), (2, 4))),
        "prev_values": normal_values(part_splits[13], (SEQS, PROP, HID), 1.0, 6.0, ((0, 4), (2, 4))),
        "prev_decay": jnp.clip(-1.0 + 0.98 * jax.random.uniform(part_splits[14], (SEQS, PROP, H), jnp.float32) ** block_levels(part_splits[14], (SEQS, PROP, H), ((0, 4), (2, 4)), -0.2, 0.2), -1.0, -0.02),
        "prev_write": jnp.clip(0.05 + 0.9 * jax.random.uniform(part_splits[15], (SEQS, PROP, H), jnp.float32) ** block_levels(part_splits[15], (SEQS, PROP, H), ((0, 4), (2, 4)), -0.2, 0.2), 0.05, 0.95),
        "accepted": plant(jax.random.randint(part_splits[16], (SEQS,), 0, PROP + 1), jax.random.fold_in(part_splits[16], 1), 0, PROP).astype(jnp.int32),
    }


EPSILON = 1e-06

def unit_rows(values):
    return values * lax.rsqrt(lax.optimization_barrier(jnp.sum(values * values, axis=-1, keepdims=True)) + EPSILON)

def update_state(state_matrix, single_key_row, value_row, decay_row, write_row):
    state_matrix = state_matrix * jnp.exp(decay_row)[:, None, None]
    draft_token = jnp.einsum('xaf,xa->xf', state_matrix, single_key_row, precision=lax.Precision.HIGHEST)
    return state_matrix + write_row[:, None, None] * single_key_row[:, :, None] * (value_row - draft_token)[:, None, :]

def one_sequence(items):
    carried_state, query_rows, keys, values, log_decay, writes, old_keys, old_values, old_decay, old_writes = items
    for token_position in range(PROP):
        carried_state = update_state(carried_state, old_keys[token_position], old_values[token_position], old_decay[token_position], old_writes[token_position])
    taken_state = carried_state
    produced_output = []
    for token_position in range(PROP):
        carried_state = update_state(carried_state, keys[token_position], values[token_position], log_decay[token_position], writes[token_position])
        produced_output.append(jnp.einsum('xaf,xa->xf', carried_state, query_rows[token_position], precision=lax.Precision.HIGHEST))
    return (taken_state, jnp.stack(produced_output))

def reference(hidden, norm_gain, w_query, w_key, w_value, w_gate, w_decay, w_write, decay_rate, head_gain, w_output, state, prev_keys, prev_values, prev_decay, prev_write, accepted):
    wide = hidden.astype(jnp.float32)
    inverse = lax.rsqrt(lax.optimization_barrier(jnp.mean(wide * wide, axis=1)) + EPSILON)
    scaled = (wide * norm_gain.astype(jnp.float32)).astype(jnp.bfloat16)
    seqs = state.shape[0]

    def project(weight):
        return jnp.dot(scaled, weight, preferred_element_type=jnp.float32) * inverse[:, None]

    def split_heads(block):
        return block.reshape(seqs, PROP, H, DK)
    query_rows = unit_rows(split_heads(project(w_query))) * DK ** (-0.5)
    keys = unit_rows(split_heads(project(w_key)))
    values = split_heads(project(w_value))
    gates = split_heads(project(w_gate))
    log_decay = (-decay_rate * jax.nn.softplus(project(w_decay))).reshape(seqs, PROP, H)
    writes = jax.nn.sigmoid(project(w_write)).reshape(seqs, PROP, H)
    taken = jnp.arange(PROP, dtype=jnp.int32)[None, :] < accepted[:, None]
    old_keys = unit_rows(split_heads(prev_keys.astype(jnp.float32)))
    old_values = split_heads(prev_values.astype(jnp.float32))
    old_decay = jnp.where(taken[:, :, None], prev_decay, 0.0)
    old_writes = jnp.where(taken[:, :, None], prev_write, 0.0)
    carried_state = state.reshape(seqs, H, DK, DK)
    taken_states, outputs = lax.map(one_sequence, (carried_state, query_rows, keys, values, log_decay, writes, old_keys, old_values, old_decay, old_writes))
    normed = outputs * lax.rsqrt(lax.optimization_barrier(jnp.mean(outputs * outputs, axis=-1, keepdims=True)) + EPSILON)
    normed = normed * head_gain.astype(jnp.float32) * jax.nn.silu(gates)
    heads_out = normed.reshape(seqs * PROP, H * DK).astype(jnp.bfloat16)
    total = jnp.dot(heads_out, w_output, preferred_element_type=jnp.float32)
    return (total.astype(jnp.bfloat16), taken_states.reshape(seqs, H, DK * DK))
```

```python
import functools

import jax
import jax.numpy as jnp
from jax import lax
from jax.experimental import pallas as pl
from jax.experimental.pallas import tpu as pltpu
from jax.sharding import PartitionSpec as P

EPSILON = 1e-06
LANES = 128
HALF = LANES // 2
exact = functools.partial(
    lax.dot_general, precision=lax.Precision.HIGHEST, preferred_element_type=jnp.float32
)
PLAIN = (((1,), (0,)), ((), ()))
BOTH_LAST = (((1,), (1,)), ((), ()))
BOTH_FIRST = (((0,), (0,)), ((), ()))
VMEM = pl.BlockSpec(memory_space=pltpu.VMEM)
ANY = pl.BlockSpec(memory_space=pl.ANY)


def unit_rows(values):
    return values * lax.rsqrt(jnp.sum(values * values, axis=-1, keepdims=True) + EPSILON)


def project_kernel(peers, heads, order, hidden, gain, small_weights, *refs):
    weights, (own, token), sends = refs[:4], refs[4:6], refs[6 : 5 + peers]
    held, total, sems = refs[5 + peers], refs[6 + peers], refs[7 + peers]
    width = weights[0].shape[1]
    copies = [pltpu.make_async_copy(w, held.at[i], sems.at[i]) for i, w in enumerate(weights)]
    for copy in copies:
        copy.start()
    wide = hidden[...].astype(jnp.float32)
    scaled = (wide * gain[...].astype(jnp.float32)).astype(jnp.bfloat16)
    small = jnp.dot(scaled, small_weights[...], preferred_element_type=jnp.float32)
    column = lax.broadcasted_iota(jnp.int32, small.shape, 1)
    squares = jnp.sum(wide * wide, axis=1, keepdims=True)
    small = jnp.where(column == 2 * heads, squares, small)
    high = small.astype(jnp.bfloat16).astype(jnp.float32)
    coded = jnp.where(column < HALF, high, pltpu.roll(small - high, HALF, 1))
    total[:, 4 * width :] = coded
    owned = own.shape[0]
    starts = [pl.multiple_of(order[s] * owned, owned) for s in range(peers)]
    for i, copy in enumerate(copies):
        copy.wait()
        columns = slice(i * width, (i + 1) * width)
        total[:, columns] = jnp.dot(scaled, held[i], preferred_element_type=jnp.float32)
        own[:, columns] = total[pl.ds(starts[0], owned), columns]
        for s in range(1, peers):
            sends[s - 1][:, columns] = total[pl.ds(starts[s], owned), columns].astype(jnp.bfloat16)
    columns = slice(4 * width, 4 * width + LANES)
    own[:, columns] = total[pl.ds(starts[0], owned), columns]
    for s in range(1, peers):
        sends[s - 1][:, columns] = total[pl.ds(starts[s], owned), columns].astype(jnp.bfloat16)
    token[...] = jnp.zeros(token.shape, token.dtype)


def block_masks(rows, proposals):
    row = lax.broadcasted_iota(jnp.int32, (rows, rows), 0)
    column = lax.broadcasted_iota(jnp.int32, (rows, rows), 1)
    same = (row // proposals) == (column // proposals)
    return same & (row >= column), same & (row > column)


def decay_terms(log_decay, lower):
    ones = jnp.where(lower, 1.0, 0.0)
    return exact(ones, log_decay, PLAIN), exact(log_decay, ones, (((0,), (1,)), ((), ())))


def solve(coupling, source, proposals):
    power = coupling
    solved = source - exact(power, source, PLAIN)
    reach = 2
    while reach < proposals:
        power = exact(power, power, PLAIN)
        solved = solved + exact(power, solved, PLAIN)
        reach *= 2
    return solved


def state_kernel(proposals, state, keys_in, values_in, decay, writes, token, state_out):
    seqs, heads, head_size, _ = state.shape
    rows = keys_in.shape[0]
    lower, strict = block_masks(rows, proposals)
    totals, totals_across = decay_terms(decay[...], lower)
    tile = 2 * proposals
    first = lax.broadcasted_iota(jnp.int32, (tile, head_size), 0) < proposals
    for h in range(heads):
        lanes = slice(h * head_size, (h + 1) * head_size)
        keys = unit_rows(keys_in[:, lanes].astype(jnp.float32))
        total = totals[:, h : h + 1]
        within = jnp.where(
            lower, jnp.exp(jnp.where(lower, total - totals_across[h : h + 1, :], 0.0)), 0.0
        )
        write = writes[:, h : h + 1]
        coupling = jnp.where(strict, write * exact(keys, keys, BOTH_LAST) * within, 0.0)
        reads = []
        for t in range(rows // tile):
            tile_keys = keys[t * tile : (t + 1) * tile]
            reads.append(
                jnp.where(
                    first,
                    exact(tile_keys, state[2 * t, h], PLAIN),
                    exact(tile_keys, state[2 * t + 1, h], PLAIN),
                )
            )
        source = write * (
            values_in[:, lanes].astype(jnp.float32)
            - jnp.exp(total) * jnp.concatenate(reads, axis=0)
        )
        fresh = solve(coupling, source, proposals)
        for s in range(seqs):
            t, upper = divmod(s, 2)
            part = slice(t * tile, (t + 1) * tile)
            last = totals[(s + 1) * proposals - 1 : (s + 1) * proposals, h : h + 1]
            mine = first if upper == 0 else jnp.logical_not(first)
            left = jnp.where(mine, last - total[part], 0.0)
            faded = jnp.where(mine, keys[part] * jnp.exp(left), 0.0)
            state_out[s, h] = state[s, h] * jnp.exp(last) + exact(faded, fresh[part], BOTH_FIRST)


def read_kernel(proposals, features, state, rate, head_gain, own, *refs):
    received, heads_out = refs[:-1], refs[-1]
    seqs, heads, head_size, _ = state.shape
    width = heads * head_size
    rows = own.shape[0]
    whole = own[...]
    for block in received:
        whole = whole + block[...].astype(jnp.float32)
    small = whole[:, 4 * width :]
    small = small + pltpu.roll(small, HALF, 1)
    inverse = lax.rsqrt(small[:, 2 * heads : 2 * heads + 1] / features + EPSILON)
    small = small * inverse
    log_decay = -rate[...] * jax.nn.softplus(small)
    strength = jax.nn.sigmoid(small)
    lower, strict = block_masks(rows, proposals)
    totals, totals_across = decay_terms(log_decay, lower)
    tile = 2 * proposals
    row = lax.broadcasted_iota(jnp.int32, (2 * tile, head_size), 0)
    first = (row % tile) < proposals
    for h in range(heads):
        q, k, v, g = (
            whole[:, i * width + h * head_size : i * width + (h + 1) * head_size] * inverse
            for i in range(4)
        )
        queries = unit_rows(q) * head_size ** (-0.5)
        keys = unit_rows(k)
        total = totals[:, h : h + 1]
        within = jnp.where(
            lower, jnp.exp(jnp.where(lower, total - totals_across[h : h + 1, :], 0.0)), 0.0
        )
        write = strength[:, heads + h : heads + h + 1]
        coupling = jnp.where(strict, write * exact(keys, keys, BOTH_LAST) * within, 0.0)
        scores = exact(queries, keys, BOTH_LAST) * within
        key_reads, query_reads = [], []
        for t in range(rows // tile):
            part = slice(t * tile, (t + 1) * tile)
            stacked = jnp.concatenate([keys[part], queries[part]], axis=0)
            both = jnp.where(
                first,
                exact(stacked, state[2 * t, h], PLAIN),
                exact(stacked, state[2 * t + 1, h], PLAIN),
            )
            key_reads.append(both[:tile])
            query_reads.append(both[tile:])
        kept = jnp.exp(total)
        source = write * (v - kept * jnp.concatenate(key_reads, axis=0))
        fresh = solve(coupling, source, proposals)
        read = kept * jnp.concatenate(query_reads, axis=0) + exact(scores, fresh, PLAIN)
        normed = read * lax.rsqrt(jnp.mean(read * read, axis=-1, keepdims=True) + EPSILON)
        normed = normed * head_gain[...].astype(jnp.float32) * (g * jax.nn.sigmoid(g))
        heads_out[:, h * head_size : (h + 1) * head_size] = normed.astype(jnp.bfloat16)


def output_kernel(peers, order, half, weight, *refs):
    blocks, (keep, send), rows = refs[:peers], refs[peers : peers + 2], refs[peers + 2]
    owned = blocks[0].shape[0]
    for s in range(peers):
        rows[pl.ds(pl.multiple_of(order[s] * owned, owned), owned), :] = blocks[s][...]
    part = keep.shape[0]
    other = pl.multiple_of((1 - half[0]) * part, part)
    mine = pl.multiple_of(half[0] * part, part)
    send[...] = jnp.dot(
        rows[pl.ds(other, part), :], weight[...], preferred_element_type=jnp.float32
    ).astype(jnp.bfloat16)
    keep[...] = jnp.dot(
        rows[pl.ds(mine, part), :], weight[...], preferred_element_type=jnp.float32
    )


def join_kernel(half, mine, theirs, out):
    part = mine.shape[0]
    out[pl.ds(pl.multiple_of(half[0] * part, part), part), :] = mine[...]
    out[pl.ds(pl.multiple_of((1 - half[0]) * part, part), part), :] = theirs[...]


def shift(array, axis, size, by):
    return lax.ppermute(array, axis, [(i, (i + by) % size) for i in range(size)])


def swap(array, axis, size, bit):
    return lax.ppermute(array, axis, [(i, i ^ bit) for i in range(size)])


def per_device(
    kv,
    tp,
    hidden,
    norm_gain,
    w_query,
    w_key,
    w_value,
    w_gate,
    w_decay,
    w_write,
    decay_rate,
    head_gain,
    w_output,
    state,
    prev_keys,
    prev_values,
    prev_decay,
    prev_write,
    accepted,
):
    f32, bf16 = jnp.float32, jnp.bfloat16
    heads = w_decay.shape[1]
    width = w_query.shape[1]
    head_size = width // heads
    tokens, local_columns = hidden.shape
    owned = tokens // kv
    seqs, proposals = prev_keys.shape[:2]
    me = lax.axis_index("kv")
    offset = me * local_columns
    to_peers = (me + jnp.arange(kv, dtype=jnp.int32)) % kv
    from_peers = (me - jnp.arange(kv, dtype=jnp.int32) + kv) % kv
    gain_part = lax.dynamic_slice_in_dim(norm_gain, offset, local_columns, 0)[None, :]
    small_weights = jnp.concatenate(
        [
            lax.dynamic_slice_in_dim(w_decay, offset, local_columns, 0),
            lax.dynamic_slice_in_dim(w_write, offset, local_columns, 0),
            jnp.zeros((local_columns, LANES - 2 * heads), bf16),
        ],
        axis=1,
    )
    smem = pl.BlockSpec(memory_space=pltpu.SMEM)
    row_width = 4 * width + LANES
    own, token, *sends = pl.pallas_call(
        functools.partial(project_kernel, kv, heads),
        out_shape=[
            jax.ShapeDtypeStruct((owned, row_width), f32),
            jax.ShapeDtypeStruct((8, LANES), f32),
        ]
        + [jax.ShapeDtypeStruct((owned, row_width), bf16)] * (kv - 1),
        in_specs=[smem, VMEM, VMEM, VMEM] + [ANY] * 4,
        out_specs=[VMEM] * (kv + 1),
        scratch_shapes=[
            pltpu.VMEM((4, local_columns, width), bf16),
            pltpu.VMEM((tokens, row_width), f32),
            pltpu.SemaphoreType.DMA((4,)),
        ],
        name="project",
    )(to_peers, hidden, gain_part, small_weights, w_query, w_key, w_value, w_gate)
    received = [shift(block, "kv", kv, s + 1) for s, block in enumerate(sends)]

    taken = jnp.arange(proposals, dtype=jnp.int32)[None, :] < accepted[:, None]
    old_decay = jnp.where(taken[:, :, None], prev_decay, 0.0).reshape(owned, heads)
    old_writes = jnp.where(taken[:, :, None], prev_write, 0.0).reshape(owned, heads)
    carried_state = pl.pallas_call(
        functools.partial(state_kernel, proposals),
        out_shape=jax.ShapeDtypeStruct((seqs, heads, head_size, head_size), f32),
        in_specs=[VMEM] * 5 + [ANY],
        out_specs=VMEM,
        name="old_state",
    )(
        state.reshape(seqs, heads, head_size, head_size),
        prev_keys.reshape(owned, width),
        prev_values.reshape(owned, width),
        old_decay,
        old_writes,
        token,
    )
    rate = jnp.concatenate([decay_rate, jnp.zeros((LANES - heads,), f32)])[None, :]
    heads_out = pl.pallas_call(
        functools.partial(read_kernel, proposals, norm_gain.shape[0]),
        out_shape=jax.ShapeDtypeStruct((owned, width), bf16),
        in_specs=[VMEM] * (3 + kv),
        out_specs=VMEM,
        name="read",
    )(carried_state, rate, head_gain[None, :], own, *received)
    gathered = [heads_out] + [shift(heads_out, "kv", kv, s) for s in range(1, kv)]
    half = (lax.axis_index("tp") % 2).astype(jnp.int32)[None]
    part = tokens // 2
    model = w_output.shape[1]
    keep, send = pl.pallas_call(
        functools.partial(output_kernel, kv),
        out_shape=[
            jax.ShapeDtypeStruct((part, model), f32),
            jax.ShapeDtypeStruct((part, model), bf16),
        ],
        in_specs=[smem, smem] + [VMEM] * (1 + kv),
        out_specs=[VMEM, VMEM],
        scratch_shapes=[pltpu.VMEM((tokens, width), bf16)],
        name="output",
    )(from_peers, half, w_output, *gathered)
    pair = keep + swap(send, "tp", tp, 1).astype(f32)
    bit = 2
    while bit < tp:
        pair = pair.astype(bf16)
        pair = pair.astype(f32) + swap(pair, "tp", tp, bit).astype(f32)
        bit *= 2
    done = pair.astype(bf16)
    mixed = pl.pallas_call(
        join_kernel,
        out_shape=jax.ShapeDtypeStruct((tokens, model), bf16),
        in_specs=[smem, VMEM, VMEM],
        out_specs=VMEM,
        name="join",
    )(half, done, swap(done, "tp", tp, 1))
    return (mixed, carried_state.reshape(seqs, heads, head_size * head_size))


def solution(mesh):
    placed = (
        P("grp", "kv"),
        P(),
        P("kv", "tp"),
        P("kv", "tp"),
        P("kv", "tp"),
        P("kv", "tp"),
        P(None, "tp"),
        P(None, "tp"),
        P("tp"),
        P(),
        P("tp", "kv"),
        P(("grp", "kv"), "tp", None),
        P(("grp", "kv"), None, "tp"),
        P(("grp", "kv"), None, "tp"),
        P(("grp", "kv"), None, "tp"),
        P(("grp", "kv"), None, "tp"),
        P(("grp", "kv")),
    )
    return jax.shard_map(
        functools.partial(per_device, mesh.shape["kv"], mesh.shape["tp"]),
        mesh=mesh,
        in_specs=placed,
        out_specs=(P("grp", "kv"), P(("grp", "kv"), "tp", None)),
        check_vma=False,
    )
```

```python
import functools

import jax
import jax.numpy as jnp
from jax import lax
from jax.experimental import pallas as pl
from jax.experimental.pallas import tpu as pltpu
from jax.sharding import PartitionSpec as P

EPSILON = 1e-06
LANES = 128
HALF = LANES // 2
exact = functools.partial(
    lax.dot_general, precision=lax.Precision.HIGHEST, preferred_element_type=jnp.float32
)
quick = functools.partial(lax.dot_general, preferred_element_type=jnp.float32)
PLAIN = (((1,), (0,)), ((), ()))
BOTH_LAST = (((1,), (1,)), ((), ()))
BOTH_FIRST = (((0,), (0,)), ((), ()))
VMEM = pl.BlockSpec(memory_space=pltpu.VMEM)
ANY = pl.BlockSpec(memory_space=pl.ANY)


def unit_rows(values):
    return values * lax.rsqrt(jnp.sum(values * values, axis=-1, keepdims=True) + EPSILON)


def project_kernel(peers, heads, hidden, gain, decay_across, write_across, *refs):
    weights, (own, token), sends = refs[:4], refs[4:6], refs[6 : 5 + peers]
    held, total, sems = refs[5 + peers], refs[6 + peers], refs[7 + peers]
    me = lax.axis_index("kv")
    depth = hidden.shape[1]
    mine = pl.ds(pl.multiple_of(me * depth, depth), depth)
    width = weights[0].shape[1]
    copies = [pltpu.make_async_copy(w, held.at[i], sems.at[i]) for i, w in enumerate(weights)]
    for copy in copies:
        copy.start()
    wide = hidden[...].astype(jnp.float32)
    scaled = (wide * gain[0:1, :]).astype(jnp.bfloat16)
    small_across = jnp.concatenate(
        [
            decay_across[:, mine].astype(jnp.float32),
            write_across[:, mine].astype(jnp.float32),
            jnp.zeros((LANES - 2 * heads, depth), jnp.float32),
        ],
        axis=0,
    ).astype(jnp.bfloat16)
    small = quick(scaled, small_across, BOTH_LAST)
    column = lax.broadcasted_iota(jnp.int32, small.shape, 1)
    squares = jnp.sum(wide * wide, axis=1, keepdims=True)
    small = jnp.where(column == 2 * heads, squares, small)
    high = small.astype(jnp.bfloat16).astype(jnp.float32)
    coded = jnp.where(column < HALF, high, pltpu.roll(small - high, HALF, 1))
    total[:, 4 * width :] = coded
    owned = own.shape[0]
    starts = [pl.multiple_of(lax.rem(me + s, peers) * owned, owned) for s in range(peers)]
    for i, copy in enumerate(copies):
        copy.wait()
        columns = slice(i * width, (i + 1) * width)
        total[:, columns] = jnp.dot(scaled, held[i], preferred_element_type=jnp.float32)
        own[:, columns] = total[pl.ds(starts[0], owned), columns]
        for s in range(1, peers):
            sends[s - 1][:, columns] = total[pl.ds(starts[s], owned), columns].astype(jnp.bfloat16)
    columns = slice(4 * width, 4 * width + LANES)
    own[:, columns] = total[pl.ds(starts[0], owned), columns]
    for s in range(1, peers):
        sends[s - 1][:, columns] = total[pl.ds(starts[s], owned), columns].astype(jnp.bfloat16)
    token[...] = jnp.zeros(token.shape, token.dtype)


def block_masks(rows, proposals):
    row = lax.broadcasted_iota(jnp.int32, (rows, rows), 0)
    column = lax.broadcasted_iota(jnp.int32, (rows, rows), 1)
    same = (row // proposals) == (column // proposals)
    return same & (row >= column), same & (row > column)


def decay_terms(log_decay, lower):
    ones = jnp.where(lower, 1.0, 0.0)
    return exact(ones, log_decay, PLAIN), exact(log_decay, ones, (((0,), (1,)), ((), ())))


def solve(coupling, source, proposals):
    power = coupling
    solved = source - quick(power, source, PLAIN)
    reach = 2
    while reach < proposals:
        power = quick(power, power, PLAIN)
        solved = solved + quick(power, solved, PLAIN)
        reach *= 2
    return solved


def state_kernel(proposals, state, keys_in, values_in, decay, writes, token, state_out):
    seqs, heads, head_size, _ = state.shape
    rows = keys_in.shape[0]
    lower, strict = block_masks(rows, proposals)
    totals, totals_across = decay_terms(decay[...], lower)
    tile = 2 * proposals
    first = lax.broadcasted_iota(jnp.int32, (tile, head_size), 0) < proposals
    for h in range(heads):
        lanes = slice(h * head_size, (h + 1) * head_size)
        keys = unit_rows(keys_in[:, lanes].astype(jnp.float32))
        total = totals[:, h : h + 1]
        within = jnp.where(
            lower, jnp.exp(jnp.where(lower, total - totals_across[h : h + 1, :], 0.0)), 0.0
        )
        write = writes[:, h : h + 1]
        coupling = jnp.where(strict, write * quick(keys, keys, BOTH_LAST) * within, 0.0)
        reads = []
        for t in range(rows // tile):
            tile_keys = keys[t * tile : (t + 1) * tile]
            reads.append(
                jnp.where(
                    first,
                    quick(tile_keys, state[2 * t, h], PLAIN),
                    quick(tile_keys, state[2 * t + 1, h], PLAIN),
                )
            )
        source = write * (
            values_in[:, lanes].astype(jnp.float32)
            - jnp.exp(total) * jnp.concatenate(reads, axis=0)
        )
        fresh = solve(coupling, source, proposals)
        for s in range(seqs):
            t, upper = divmod(s, 2)
            part = slice(t * tile, (t + 1) * tile)
            last = totals[(s + 1) * proposals - 1 : (s + 1) * proposals, h : h + 1]
            mine = first if upper == 0 else jnp.logical_not(first)
            left = jnp.where(mine, last - total[part], 0.0)
            faded = jnp.where(mine, keys[part] * jnp.exp(left), 0.0)
            state_out[s, h] = state[s, h] * jnp.exp(last) + quick(faded, fresh[part], BOTH_FIRST)


def read_kernel(proposals, features, state_in, rate, head_gain, own, *refs):
    received, (heads_out, state, sem) = refs[:-3], refs[-3:]
    copy = pltpu.make_async_copy(state_in, state, sem)
    copy.start()
    seqs, heads, head_size, _ = state.shape
    width = heads * head_size
    rows = own.shape[0]
    whole = own[...]
    for block in received:
        whole = whole + block[...].astype(jnp.float32)
    small = whole[:, 4 * width :]
    small = small + pltpu.roll(small, HALF, 1)
    inverse = lax.rsqrt(small[:, 2 * heads : 2 * heads + 1] / features + EPSILON)
    small = small * inverse
    log_decay = -rate[...] * jax.nn.softplus(small)
    strength = jax.nn.sigmoid(small)
    lower, strict = block_masks(rows, proposals)
    totals, totals_across = decay_terms(log_decay, lower)
    tile = 2 * proposals
    row = lax.broadcasted_iota(jnp.int32, (2 * tile, head_size), 0)
    first = (row % tile) < proposals
    copy.wait()
    for h in range(heads):
        q, k, v, g = (
            whole[:, i * width + h * head_size : i * width + (h + 1) * head_size] * inverse
            for i in range(4)
        )
        queries = unit_rows(q) * head_size ** (-0.5)
        keys = unit_rows(k)
        total = totals[:, h : h + 1]
        within = jnp.where(
            lower, jnp.exp(jnp.where(lower, total - totals_across[h : h + 1, :], 0.0)), 0.0
        )
        write = strength[:, heads + h : heads + h + 1]
        coupling = jnp.where(strict, write * quick(keys, keys, BOTH_LAST) * within, 0.0)
        scores = quick(queries, keys, BOTH_LAST) * within
        key_reads, query_reads = [], []
        for t in range(rows // tile):
            part = slice(t * tile, (t + 1) * tile)
            stacked = jnp.concatenate([keys[part], queries[part]], axis=0)
            both = jnp.where(
                first,
                quick(stacked, state[2 * t, h], PLAIN),
                quick(stacked, state[2 * t + 1, h], PLAIN),
            )
            key_reads.append(both[:tile])
            query_reads.append(both[tile:])
        kept = jnp.exp(total)
        source = write * (v - kept * jnp.concatenate(key_reads, axis=0))
        fresh = solve(coupling, source, proposals)
        read = kept * jnp.concatenate(query_reads, axis=0) + quick(scores, fresh, PLAIN)
        normed = read * lax.rsqrt(jnp.mean(read * read, axis=-1, keepdims=True) + EPSILON)
        normed = normed * head_gain[...].astype(jnp.float32) * (g * jax.nn.sigmoid(g))
        heads_out[:, h * head_size : (h + 1) * head_size] = normed.astype(jnp.bfloat16)


def shift(array, axis, size, by):
    return lax.ppermute(array, axis, [(i, (i + by) % size) for i in range(size)])


def swap(array, axis, size, bit):
    return lax.ppermute(array, axis, [(i, i ^ bit) for i in range(size)])


def per_device(
    kv,
    tp,
    hidden,
    norm_gain,
    w_query,
    w_key,
    w_value,
    w_gate,
    w_decay,
    w_write,
    decay_rate,
    head_gain,
    w_output,
    state,
    prev_keys,
    prev_values,
    prev_decay,
    prev_write,
    accepted,
):
    f32, bf16 = jnp.float32, jnp.bfloat16
    heads = w_decay.shape[1]
    width = w_query.shape[1]
    head_size = width // heads
    tokens, local_columns = hidden.shape
    owned = tokens // kv
    seqs, proposals = prev_keys.shape[:2]
    me = lax.axis_index("kv")
    offset = me * local_columns
    gain_part = lax.dynamic_slice_in_dim(norm_gain, offset, local_columns, 0).astype(f32)
    gain_part = jnp.broadcast_to(gain_part[None, :], (8, local_columns))
    row_width = 4 * width + LANES
    own, token, *sends = pl.pallas_call(
        functools.partial(project_kernel, kv, heads),
        out_shape=[
            jax.ShapeDtypeStruct((owned, row_width), f32),
            jax.ShapeDtypeStruct((8, LANES), f32),
        ]
        + [jax.ShapeDtypeStruct((owned, row_width), bf16)] * (kv - 1),
        in_specs=[VMEM] * 4 + [ANY] * 4,
        out_specs=[VMEM] * (kv + 1),
        scratch_shapes=[
            pltpu.VMEM((4, local_columns, width), bf16),
            pltpu.VMEM((tokens, row_width), f32),
            pltpu.SemaphoreType.DMA((4,)),
        ],
        name="project",
    )(hidden, gain_part, w_decay.T, w_write.T, w_query, w_key, w_value, w_gate)
    received = [shift(block, "kv", kv, s + 1) for s, block in enumerate(sends)]

    taken = jnp.arange(proposals, dtype=jnp.int32)[None, :] < accepted[:, None]
    old_decay = jnp.where(taken[:, :, None], prev_decay, 0.0).reshape(owned, heads)
    old_writes = jnp.where(taken[:, :, None], prev_write, 0.0).reshape(owned, heads)
    carried_state = pl.pallas_call(
        functools.partial(state_kernel, proposals),
        out_shape=jax.ShapeDtypeStruct((seqs, heads, head_size, head_size), f32),
        in_specs=[VMEM] * 5 + [ANY],
        out_specs=VMEM,
        name="old_state",
    )(
        state.reshape(seqs, heads, head_size, head_size),
        prev_keys.reshape(owned, width),
        prev_values.reshape(owned, width),
        old_decay,
        old_writes,
        token,
    )
    rate = jnp.concatenate([decay_rate, jnp.zeros((LANES - heads,), f32)])[None, :]
    heads_out = pl.pallas_call(
        functools.partial(read_kernel, proposals, norm_gain.shape[0]),
        out_shape=jax.ShapeDtypeStruct((owned, width), bf16),
        in_specs=[ANY] + [VMEM] * (2 + kv),
        out_specs=VMEM,
        scratch_shapes=[
            pltpu.VMEM((seqs, heads, head_size, head_size), f32),
            pltpu.SemaphoreType.DMA,
        ],
        name="read",
    )(carried_state, rate, head_gain[None, :], own, *received)
    gathered = [heads_out] + [shift(heads_out, "kv", kv, kv - s) for s in range(1, kv)]
    half = lax.axis_index("tp") & 1
    part = tokens // 2
    twice = jnp.concatenate(gathered + gathered, axis=0)
    origin = lax.rem(kv - me, kv) * owned

    def half_product(which):
        rows = lax.dynamic_slice_in_dim(twice, origin + which * part, part, 0)
        return jnp.dot(rows, w_output, preferred_element_type=f32)

    send = half_product(1 - half).astype(bf16)
    keep = half_product(half)
    pair = keep + swap(send, "tp", tp, 1).astype(f32)
    bit = 2
    while bit < tp:
        pair = pair.astype(bf16)
        pair = pair.astype(f32) + swap(pair, "tp", tp, bit).astype(f32)
        bit *= 2
    done = pair.astype(bf16)
    theirs = swap(done, "tp", tp, 1)
    mixed = jnp.where(
        half == 0,
        jnp.concatenate([done, theirs], axis=0),
        jnp.concatenate([theirs, done], axis=0),
    )
    return (mixed, carried_state.reshape(seqs, heads, head_size * head_size))


def solution(mesh):
    placed = (
        P("grp", "kv"),
        P(),
        P("kv", "tp"),
        P("kv", "tp"),
        P("kv", "tp"),
        P("kv", "tp"),
        P(None, "tp"),
        P(None, "tp"),
        P("tp"),
        P(),
        P("tp", "kv"),
        P(("grp", "kv"), "tp", None),
        P(("grp", "kv"), None, "tp"),
        P(("grp", "kv"), None, "tp"),
        P(("grp", "kv"), None, "tp"),
        P(("grp", "kv"), None, "tp"),
        P(("grp", "kv")),
    )
    return jax.shard_map(
        functools.partial(per_device, mesh.shape["kv"], mesh.shape["tp"]),
        mesh=mesh,
        in_specs=placed,
        out_specs=(P("grp", "kv"), P(("grp", "kv"), "tp", None)),
        check_vma=False,
    )
```

```python
import functools

import jax
import jax.numpy as jnp
from jax import lax
from jax.experimental import pallas as pl
from jax.experimental.pallas import tpu as pltpu
from jax.sharding import PartitionSpec as P

EPSILON = 1e-06
LANES = 128
HALF = LANES // 2
exact = functools.partial(
    lax.dot_general, precision=lax.Precision.HIGHEST, preferred_element_type=jnp.float32
)
quick = functools.partial(lax.dot_general, preferred_element_type=jnp.float32)
PLAIN = (((1,), (0,)), ((), ()))
BOTH_LAST = (((1,), (1,)), ((), ()))
BOTH_FIRST = (((0,), (0,)), ((), ()))
VMEM = pl.BlockSpec(memory_space=pltpu.VMEM)
ANY = pl.BlockSpec(memory_space=pl.ANY)


def unit_rows(values):
    return values * lax.rsqrt(jnp.sum(values * values, axis=-1, keepdims=True) + EPSILON)


def project_kernel(peers, heads, hidden, gain, decay_across, write_across, *refs):
    weights, (own, token), sends = refs[:4], refs[4:6], refs[6 : 5 + peers]
    held, total, sems = refs[5 + peers], refs[6 + peers], refs[7 + peers]
    me = lax.axis_index("kv")
    depth = hidden.shape[1]
    mine = pl.ds(pl.multiple_of(me * depth, depth), depth)
    width = weights[0].shape[1]
    copies = [pltpu.make_async_copy(w, held.at[i], sems.at[i]) for i, w in enumerate(weights)]
    for copy in copies:
        copy.start()
    wide = hidden[...].astype(jnp.float32)
    scaled = (wide * gain[:, mine].astype(jnp.float32)).astype(jnp.bfloat16)
    small_across = jnp.concatenate(
        [
            decay_across[:, mine].astype(jnp.float32),
            write_across[:, mine].astype(jnp.float32),
            jnp.zeros((LANES - 2 * heads, depth), jnp.float32),
        ],
        axis=0,
    ).astype(jnp.bfloat16)
    small = quick(scaled, small_across, BOTH_LAST)
    column = lax.broadcasted_iota(jnp.int32, small.shape, 1)
    squares = jnp.sum(wide * wide, axis=1, keepdims=True)
    small = jnp.where(column == 2 * heads, squares, small)
    high = small.astype(jnp.bfloat16).astype(jnp.float32)
    coded = jnp.where(column < HALF, high, pltpu.roll(small - high, HALF, 1))
    total[:, 4 * width :] = coded
    owned = own.shape[0]
    starts = [pl.multiple_of(lax.rem(me + s, peers) * owned, owned) for s in range(peers)]
    for i, copy in enumerate(copies):
        copy.wait()
        columns = slice(i * width, (i + 1) * width)
        total[:, columns] = jnp.dot(scaled, held[i], preferred_element_type=jnp.float32)
        own[:, columns] = total[pl.ds(starts[0], owned), columns]
        for s in range(1, peers):
            sends[s - 1][:, columns] = total[pl.ds(starts[s], owned), columns].astype(jnp.bfloat16)
    columns = slice(4 * width, 4 * width + LANES)
    own[:, columns] = total[pl.ds(starts[0], owned), columns]
    for s in range(1, peers):
        sends[s - 1][:, columns] = total[pl.ds(starts[s], owned), columns].astype(jnp.bfloat16)
    token[...] = jnp.zeros(token.shape, token.dtype)


def block_masks(rows, proposals):
    row = lax.broadcasted_iota(jnp.int32, (rows, rows), 0)
    column = lax.broadcasted_iota(jnp.int32, (rows, rows), 1)
    same = (row // proposals) == (column // proposals)
    return same & (row >= column), same & (row > column)


def decay_terms(log_decay, lower):
    ones = jnp.where(lower, 1.0, 0.0)
    return exact(ones, log_decay, PLAIN), exact(log_decay, ones, (((0,), (1,)), ((), ())))


def solve(coupling, source, proposals):
    power = coupling
    solved = source - quick(power, source, PLAIN)
    reach = 2
    while reach < proposals:
        power = quick(power, power, PLAIN)
        solved = solved + quick(power, solved, PLAIN)
        reach *= 2
    return solved


def spread_rows(across, accepted, rows):
    proposals, heads, seqs = across.shape
    row = lax.broadcasted_iota(jnp.int32, (rows, seqs), 0)
    column = lax.broadcasted_iota(jnp.int32, (rows, seqs), 1)
    total = None
    for p in range(proposals):
        place = jnp.where(row == column * proposals + p, 1.0, 0.0)
        term = exact(place, jnp.where(p < accepted, across[p], 0.0), BOTH_LAST)
        total = term if total is None else total + term
    return total


def state_kernel(
    proposals, counts, state_in, keys_in, values_in, decay, writes, token, out, *scratch
):
    state, state_out, in_sems, out_sems = scratch
    seqs, heads, head_size, _ = state.shape
    loads = [
        pltpu.make_async_copy(state_in.at[:, h], state.at[:, h], in_sems.at[h])
        for h in range(heads)
    ]
    stores = [
        pltpu.make_async_copy(state_out.at[:, h], out.at[:, h], out_sems.at[h])
        for h in range(heads)
    ]
    for copy in loads:
        copy.start()
    rows = seqs * proposals
    column = lax.broadcasted_iota(jnp.int32, (heads, seqs), 1)
    accepted = jnp.zeros((heads, seqs), jnp.int32)
    for s in range(seqs):
        accepted = jnp.where(column == s, counts[s], accepted)
    lower, strict = block_masks(rows, proposals)
    totals, totals_across = decay_terms(spread_rows(decay, accepted, rows), lower)
    old_writes = spread_rows(writes, accepted, rows)
    tile = 2 * proposals
    first = lax.broadcasted_iota(jnp.int32, (tile, head_size), 0) < proposals
    for h in range(heads):
        lanes = slice(h * head_size, (h + 1) * head_size)
        keys = unit_rows(keys_in[:, :, lanes].astype(jnp.float32).reshape(rows, head_size))
        total = totals[:, h : h + 1]
        within = jnp.where(
            lower, jnp.exp(jnp.where(lower, total - totals_across[h : h + 1, :], 0.0)), 0.0
        )
        write = old_writes[:, h : h + 1]
        coupling = jnp.where(strict, write * quick(keys, keys, BOTH_LAST) * within, 0.0)
        loads[h].wait()
        reads = []
        for t in range(rows // tile):
            tile_keys = keys[t * tile : (t + 1) * tile]
            reads.append(
                jnp.where(
                    first,
                    quick(tile_keys, state[2 * t, h], PLAIN),
                    quick(tile_keys, state[2 * t + 1, h], PLAIN),
                )
            )
        source = write * (
            values_in[:, :, lanes].astype(jnp.float32).reshape(rows, head_size)
            - jnp.exp(total) * jnp.concatenate(reads, axis=0)
        )
        fresh = solve(coupling, source, proposals)
        for s in range(seqs):
            t, upper = divmod(s, 2)
            part = slice(t * tile, (t + 1) * tile)
            last = totals[(s + 1) * proposals - 1 : (s + 1) * proposals, h : h + 1]
            mine = first if upper == 0 else jnp.logical_not(first)
            left = jnp.where(mine, last - total[part], 0.0)
            faded = jnp.where(mine, keys[part] * jnp.exp(left), 0.0)
            state_out[s, h] = state[s, h] * jnp.exp(last) + quick(faded, fresh[part], BOTH_FIRST)
        stores[h].start()
    for copy in stores:
        copy.wait()


def read_kernel(proposals, features, state_in, rate, head_gain, own, *refs):
    received, (heads_out, state, sems) = refs[:-3], refs[-3:]
    seqs, heads, head_size, _ = state.shape
    loads = [
        pltpu.make_async_copy(state_in.at[:, h], state.at[:, h], sems.at[h]) for h in range(heads)
    ]
    for copy in loads:
        copy.start()
    width = heads * head_size
    rows = own.shape[0]
    whole = own[...]
    for block in received:
        whole = whole + block[...].astype(jnp.float32)
    small = whole[:, 4 * width :]
    small = small + pltpu.roll(small, HALF, 1)
    inverse = lax.rsqrt(small[:, 2 * heads : 2 * heads + 1] / features + EPSILON)
    small = small * inverse
    column = lax.broadcasted_iota(jnp.int32, (1, LANES), 1)
    rates = jnp.zeros((1, LANES), jnp.float32)
    for h in range(heads):
        rates = jnp.where(column == h, rate[h], rates)
    log_decay = -rates * jax.nn.softplus(small)
    strength = jax.nn.sigmoid(small)
    lower, strict = block_masks(rows, proposals)
    totals, totals_across = decay_terms(log_decay, lower)
    tile = 2 * proposals
    row = lax.broadcasted_iota(jnp.int32, (2 * tile, head_size), 0)
    first = (row % tile) < proposals
    for h in range(heads):
        q, k, v, g = (
            whole[:, i * width + h * head_size : i * width + (h + 1) * head_size] * inverse
            for i in range(4)
        )
        queries = unit_rows(q) * head_size ** (-0.5)
        keys = unit_rows(k)
        total = totals[:, h : h + 1]
        within = jnp.where(
            lower, jnp.exp(jnp.where(lower, total - totals_across[h : h + 1, :], 0.0)), 0.0
        )
        write = strength[:, heads + h : heads + h + 1]
        coupling = jnp.where(strict, write * quick(keys, keys, BOTH_LAST) * within, 0.0)
        scores = quick(queries, keys, BOTH_LAST) * within
        loads[h].wait()
        key_reads, query_reads = [], []
        for t in range(rows // tile):
            part = slice(t * tile, (t + 1) * tile)
            stacked = jnp.concatenate([keys[part], queries[part]], axis=0)
            both = jnp.where(
                first,
                quick(stacked, state[2 * t, h], PLAIN),
                quick(stacked, state[2 * t + 1, h], PLAIN),
            )
            key_reads.append(both[:tile])
            query_reads.append(both[tile:])
        kept = jnp.exp(total)
        source = write * (v - kept * jnp.concatenate(key_reads, axis=0))
        fresh = solve(coupling, source, proposals)
        read = kept * jnp.concatenate(query_reads, axis=0) + quick(scores, fresh, PLAIN)
        normed = read * lax.rsqrt(jnp.mean(read * read, axis=-1, keepdims=True) + EPSILON)
        normed = normed * head_gain[...].astype(jnp.float32) * (g * jax.nn.sigmoid(g))
        heads_out[:, h * head_size : (h + 1) * head_size] = normed.astype(jnp.bfloat16)


def shift(array, axis, size, by):
    return lax.ppermute(array, axis, [(i, (i + by) % size) for i in range(size)])


def swap(array, axis, size, bit):
    return lax.ppermute(array, axis, [(i, i ^ bit) for i in range(size)])


def per_device(
    kv,
    tp,
    hidden,
    norm_gain,
    w_query,
    w_key,
    w_value,
    w_gate,
    w_decay,
    w_write,
    decay_rate,
    head_gain,
    w_output,
    state,
    prev_keys,
    prev_values,
    prev_decay,
    prev_write,
    accepted,
):
    f32, bf16 = jnp.float32, jnp.bfloat16
    heads = w_decay.shape[1]
    width = w_query.shape[1]
    head_size = width // heads
    tokens, local_columns = hidden.shape
    owned = tokens // kv
    seqs, proposals = prev_keys.shape[:2]
    me = lax.axis_index("kv")
    row_width = 4 * width + LANES
    own, token, *sends = pl.pallas_call(
        functools.partial(project_kernel, kv, heads),
        out_shape=[
            jax.ShapeDtypeStruct((owned, row_width), f32),
            jax.ShapeDtypeStruct((8, LANES), f32),
        ]
        + [jax.ShapeDtypeStruct((owned, row_width), bf16)] * (kv - 1),
        in_specs=[VMEM] * 4 + [ANY] * 4,
        out_specs=[VMEM] * (kv + 1),
        scratch_shapes=[
            pltpu.VMEM((4, local_columns, width), bf16),
            pltpu.VMEM((tokens, row_width), f32),
            pltpu.SemaphoreType.DMA((4,)),
        ],
        name="project",
    )(hidden, norm_gain[None, :], w_decay.T, w_write.T, w_query, w_key, w_value, w_gate)
    received = [shift(block, "kv", kv, s + 1) for s, block in enumerate(sends)]

    smem = pl.BlockSpec(memory_space=pltpu.SMEM)
    states = pltpu.VMEM((seqs, heads, head_size, head_size), f32)
    head_sems = pltpu.SemaphoreType.DMA((heads,))
    carried_state = pl.pallas_call(
        functools.partial(state_kernel, proposals),
        out_shape=jax.ShapeDtypeStruct((seqs, heads, head_size, head_size), f32),
        in_specs=[smem, ANY] + [VMEM] * 4 + [ANY],
        out_specs=ANY,
        scratch_shapes=[states, states, head_sems, head_sems],
        name="old_state",
    )(
        accepted,
        state.reshape(seqs, heads, head_size, head_size),
        prev_keys,
        prev_values,
        prev_decay.transpose(1, 2, 0),
        prev_write.transpose(1, 2, 0),
        token,
    )
    heads_out = pl.pallas_call(
        functools.partial(read_kernel, proposals, norm_gain.shape[0]),
        out_shape=jax.ShapeDtypeStruct((owned, width), bf16),
        in_specs=[ANY, smem] + [VMEM] * (1 + kv),
        out_specs=VMEM,
        scratch_shapes=[
            states,
            head_sems,
        ],
        name="read",
    )(carried_state, decay_rate, head_gain[None, :], own, *received)
    gathered = [heads_out] + [shift(heads_out, "kv", kv, kv - s) for s in range(1, kv)]
    half = lax.axis_index("tp") & 1
    part = tokens // 2
    twice = jnp.concatenate(gathered + gathered, axis=0)
    origin = lax.rem(kv - me, kv) * owned

    def half_product(which):
        rows = lax.dynamic_slice_in_dim(twice, origin + which * part, part, 0)
        return jnp.dot(rows, w_output, preferred_element_type=f32)

    send = half_product(1 - half).astype(bf16)
    keep = half_product(half)
    pair = keep + swap(send, "tp", tp, 1).astype(f32)
    bit = 2
    while bit < tp:
        pair = pair.astype(bf16)
        pair = pair.astype(f32) + swap(pair, "tp", tp, bit).astype(f32)
        bit *= 2
    done = pair.astype(bf16)
    theirs = swap(done, "tp", tp, 1)
    mixed = jnp.where(
        half == 0,
        jnp.concatenate([done, theirs], axis=0),
        jnp.concatenate([theirs, done], axis=0),
    )
    return (mixed, carried_state.reshape(seqs, heads, head_size * head_size))


def solution(mesh):
    placed = (
        P("grp", "kv"),
        P(),
        P("kv", "tp"),
        P("kv", "tp"),
        P("kv", "tp"),
        P("kv", "tp"),
        P(None, "tp"),
        P(None, "tp"),
        P("tp"),
        P(),
        P("tp", "kv"),
        P(("grp", "kv"), "tp", None),
        P(("grp", "kv"), None, "tp"),
        P(("grp", "kv"), None, "tp"),
        P(("grp", "kv"), None, "tp"),
        P(("grp", "kv"), None, "tp"),
        P(("grp", "kv")),
    )
    return jax.shard_map(
        functools.partial(per_device, mesh.shape["kv"], mesh.shape["tp"]),
        mesh=mesh,
        in_specs=placed,
        out_specs=(P("grp", "kv"), P(("grp", "kv"), "tp", None)),
        check_vma=False,
    )
```
